32 devices in a mesh: sp: 8 (over z, x), tp: 4 (over y, core).
Axes of the slice: x: 2, y: 2, z: 4, core: 2. Of those that a mesh axis runs over, the one named last changes fastest.
Arguments:
- tokens: bfloat16 [3072, 2048], P('sp', 'tp'), may hold values from -6 to 6
- pre_gain: float32 [2048], replicated, may hold values from 0.1 to 1.9
- outer_gate_weight: bfloat16 [2048, 1024], P(None, 'tp'), may hold values from -0.125 to 0.125
- inner_gate_weight: bfloat16 [2048, 1024], P(None, 'tp'), may hold values from -0.125 to 0.125
- source_weight: bfloat16 [2048, 1024], P(None, 'tp'), may hold values from -0.125 to 0.125
- conv_taps: bfloat16 [3, 1024], P(None, 'tp'), may hold values from -3.5 to 3.5
- q_down_weight: bfloat16 [2048, 768], replicated, may hold values from -0.125 to 0.125
- q_norm_gain: float32 [768], replicated, may hold values from 0.5 to 16
- q_up_weight: bfloat16 [768, 3072], P(None, 'tp'), may hold values from -0.21875 to 0.21875
- kv_down_weight: bfloat16 [2048, 512], replicated, may hold values from -0.125 to 0.125
- rope_key_weight: bfloat16 [2048, 32], replicated, may hold values from -0.125 to 0.125
- kv_norm_gain: float32 [512], replicated, may hold values from 0.5 to 16
- kv_up_weight: bfloat16 [512, 4096], P(None, 'tp'), may hold values from -0.25 to 0.25
- attn_out_weight: bfloat16 [2048, 2048], P('tp'), may hold values from -4 to 4
- conv_out_weight: bfloat16 [1024, 2048], P('tp'), may hold values from -0.1875 to 0.1875
- post_gain: float32 [2048], P('tp'), may hold values from 0.1 to 1.9
Outputs:
- mixed: bfloat16 [3072, 2048], P('sp', 'tp')
- log_total: float32 [32, 3072], P('tp', 'sp')
The draws below stay inside these ranges and needn't reach their ends.
All inputs are finite; a program needn't handle non-finite values.
Results may differ from the reference program's by a relative error of at most 0.017.
The reference program's roundings to bfloat16 on the way count: a program that leaves them out, or rounds other values in their place, can miss the bound.
Values may be sent and summed in bfloat16 or wider, within the bound.
No kernel may reach another device: no remote copies, remote signals or barrier semaphores. Data moves between devices by JAX's collectives and lax.ppermute only.
A program may use at most 128 MiB of HBM per device.

```python
import jax
import jax.numpy as jnp
from jax import lax

D = 2048
HEADS = 32
NOPE = 64
ROPE = 32
VDIM = 64
Q_RANK = 768
KV_RANK = 512
CONV_W = 1024
TAPS = 3
TOK_DEV = 384
TOKENS = 3072
N_SP = 8
N_TP = 4


def latent_gain(key, count):
    upper = 2.0
    return jnp.exp(jax.random.uniform(key, (count,), jnp.float32, jnp.log(0.5), jnp.log(upper)))


def draw_q_norm_gain(key, part):
    return latent_gain(jax.random.fold_in(key, 11), Q_RANK)


def draw_kv_norm_gain(key, part):
    return latent_gain(jax.random.fold_in(key, 23), KV_RANK)


def block_levels(stream_key, shape, shards, low, high):
    gain, own = 1.0, jax.random.fold_in(stream_key, 6)
    for dim, parts in shards:
        steps = jnp.exp(jax.random.uniform(jax.random.fold_in(own, dim), (parts,), jnp.float32, low / len(shards), high / len(shards)))
        gain = gain * jnp.repeat(steps, shape[dim] // parts).reshape([-1 if axis == dim else 1 for axis in range(len(shape))])
    return gain


def centred(stream_key, dims, scale, bound, split=(), held_as=jnp.bfloat16):
    values = scale * jax.random.normal(stream_key, dims, jnp.float32)
    if split:
        values = values * block_levels(stream_key, dims, split, -0.22, 0.18)
    return jnp.clip(values, -bound, bound).astype(held_as)


def setup_inputs(seed: int = 0) -> dict:
    splits = jax.random.split(jax.random.key(seed), 17)
    return {
        "tokens": centred(splits[0], (TOKENS, D), 1.0, 6.0, ((0, 8), (1, 4))),
        "pre_gain": jnp.clip(1.0 + 0.18 * jax.random.normal(splits[1], (D,), jnp.float32), 0.1, 1.9),
        "outer_gate_weight": centred(splits[2], (D, CONV_W), D ** -0.5, 0.125, ((1, 4),)),
        "inner_gate_weight": centred(splits[3], (D, CONV_W), D ** -0.5, 0.125, ((1, 4),)),
        "source_weight": centred(splits[4], (D, CONV_W), D ** -0.5, 0.125, ((1, 4),)),
        "conv_taps": centred(splits[5], (TAPS, CONV_W), TAPS ** -0.5, 3.5, ((1, 4),)),
        "q_down_weight": centred(splits[6], (D, Q_RANK), D ** -0.5, 0.125),
        "q_norm_gain": draw_q_norm_gain(jax.random.fold_in(splits[16], 71), 0),
        "q_up_weight": centred(splits[8], (Q_RANK, HEADS * (NOPE + ROPE)), Q_RANK ** -0.5, 0.21875, ((1, 4),)),
        "kv_down_weight": centred(splits[9], (D, KV_RANK), D ** -0.5, 0.125),
        "rope_key_weight": centred(splits[10], (D, ROPE), D ** -0.5, 0.125),
        "kv_norm_gain": draw_kv_norm_gain(jax.random.fold_in(splits[16], 71), 0),
        "kv_up_weight": centred(splits[12], (KV_RANK, HEADS * (NOPE + VDIM)), KV_RANK ** -0.5, 0.25, ((1, 4),)),
        "attn_out_weight": centred(splits[13], (HEADS * VDIM, D), 2 ** -0.5, 4.0, ((0, 4),)),
        "conv_out_weight": centred(splits[14], (CONV_W, D), CONV_W ** -0.5, 0.1875, ((0, 4),)),
        "post_gain": jnp.clip(1.0 + 0.18 * jax.random.normal(splits[15], (D,), jnp.float32), 0.1, 1.9),
    }


EPSILON = 1e-06
THETA = 500000.0

def rms_scale(values):
    return lax.rsqrt(lax.optimization_barrier(jnp.mean(values * values, axis=-1, keepdims=True)) + EPSILON)

def rotation(positions, width):
    freqs = THETA ** (-jnp.arange(0, width, 2, dtype=jnp.float32) / width)
    angles = positions.astype(jnp.float32)[:, None] * freqs[None, :]
    return (jnp.cos(angles), jnp.sin(angles))

def rotate(values, cosine, sine):
    half = values.shape[-1] // 2
    first = values[..., :half]
    second = values[..., half:]
    return jnp.concatenate([first * cosine - second * sine, second * cosine + first * sine], axis=-1)

def reference(tokens, pre_gain, outer_gate_weight, inner_gate_weight, source_weight, conv_taps, q_down_weight, q_norm_gain, q_up_weight, kv_down_weight, rope_key_weight, kv_norm_gain, kv_up_weight, attn_out_weight, conv_out_weight, post_gain):
    wide = tokens.astype(jnp.float32)
    scaled = (wide * pre_gain).astype(jnp.bfloat16)
    factor = rms_scale(wide)

    def project(weight):
        return jnp.dot(scaled, weight, preferred_element_type=jnp.float32) * factor
    outer = project(outer_gate_weight).astype(jnp.bfloat16)
    inner = project(inner_gate_weight).astype(jnp.bfloat16)
    source = project(source_weight).astype(jnp.bfloat16)
    driven = (inner.astype(jnp.float32) * source.astype(jnp.float32)).astype(jnp.bfloat16)
    padded = jnp.concatenate([jnp.zeros((TAPS - 1, CONV_W), jnp.bfloat16), driven], axis=0)
    convolved = jnp.zeros((TOKENS, CONV_W), jnp.float32)
    for index in range(TAPS):
        convolved = convolved + conv_taps[index].astype(jnp.float32) * padded[index:index + TOKENS].astype(jnp.float32)
    conv_branch = (outer.astype(jnp.float32) * convolved).astype(jnp.bfloat16)
    positions = jnp.arange(TOKENS, dtype=jnp.int32)
    cosine, sine = rotation(positions, ROPE)
    q_latent = project(q_down_weight)
    q_normed = (q_latent * rms_scale(q_latent) * q_norm_gain).astype(jnp.bfloat16)
    query = jnp.dot(q_normed, q_up_weight, preferred_element_type=jnp.float32).reshape(TOKENS, HEADS, NOPE + ROPE)
    q_plain = query[..., :NOPE].astype(jnp.bfloat16)
    q_turned = rotate(query[..., NOPE:], cosine[:, None], sine[:, None]).astype(jnp.bfloat16)
    kv_latent = project(kv_down_weight)
    latent = (kv_latent * rms_scale(kv_latent) * kv_norm_gain).astype(jnp.bfloat16)
    rope_key = rotate(project(rope_key_weight), cosine, sine).astype(jnp.bfloat16)
    keyvals = jnp.dot(latent, kv_up_weight, preferred_element_type=jnp.float32).astype(jnp.bfloat16)
    keyvals = keyvals.reshape(TOKENS, HEADS, NOPE + VDIM)
    head_plain = jnp.transpose(q_plain, (1, 0, 2))
    head_turned = jnp.transpose(q_turned, (1, 0, 2))
    head_keys = jnp.transpose(keyvals[..., :NOPE], (1, 0, 2))
    head_values = jnp.transpose(keyvals[..., NOPE:], (1, 0, 2))
    scale = (NOPE + ROPE) ** (-0.5)
    outputs = []
    logs = []
    for block in range(N_SP):
        first = block * TOK_DEV
        last = first + TOK_DEV
        key_turned = rope_key[:last]
        query_pos = jnp.arange(first, last, dtype=jnp.int32)
        key_pos = jnp.arange(last, dtype=jnp.int32)
        allowed = key_pos[None, :] <= query_pos[:, None]

        def per_head(items):
            plain, turned, keys, values = items
            scores = jnp.dot(plain, keys.T, preferred_element_type=jnp.float32)
            scores = scores + jnp.dot(turned, key_turned.T, preferred_element_type=jnp.float32)
            scores = jnp.where(allowed, scores * scale, -jnp.inf)
            maxima = lax.optimization_barrier(jnp.max(scores, axis=-1, keepdims=True))
            weights = jnp.exp(scores - maxima)
            totals = lax.optimization_barrier(jnp.sum(weights, axis=-1))
            result = jnp.dot(weights.astype(jnp.bfloat16), values, preferred_element_type=jnp.float32) / totals[:, None]
            return (result.astype(jnp.bfloat16), maxima[:, 0] + jnp.log(totals))
        block_out, block_log = lax.map(per_head, (head_plain[:, first:last], head_turned[:, first:last], head_keys[:, :last], head_values[:, :last]))
        outputs.append(block_out)
        logs.append(block_log)
    attended = jnp.concatenate(outputs, axis=1)
    log_total = jnp.concatenate(logs, axis=1)
    attended = jnp.transpose(attended, (1, 0, 2)).reshape(TOKENS, HEADS * VDIM)
    head_rows = HEADS // N_TP * VDIM
    channel_rows = CONV_W // N_TP
    projected = jnp.zeros((TOKENS, D), jnp.float32)
    for group in range(N_TP):
        head_part = jnp.dot(attended[:, group * head_rows:(group + 1) * head_rows], attn_out_weight[group * head_rows:(group + 1) * head_rows], preferred_element_type=jnp.float32)
        conv_part = jnp.dot(conv_branch[:, group * channel_rows:(group + 1) * channel_rows], conv_out_weight[group * channel_rows:(group + 1) * channel_rows], preferred_element_type=jnp.float32)
        rounded = lax.optimization_barrier((head_part + conv_part).astype(jnp.bfloat16))
        projected = projected + rounded.astype(jnp.float32)
    mixed = (projected * rms_scale(projected) * post_gain).astype(jnp.bfloat16)
    return (mixed, log_total)
```

```python
import functools
import math

import jax
import jax.numpy as jnp
from jax import lax
from jax.experimental import pallas as pl
from jax.experimental.pallas import tpu as pltpu
from jax.sharding import PartitionSpec as P

NOPE = 64
ROPE = 32
VDIM = 64
TAPS = 3
EPSILON = 1e-06
THETA = 500000.0
NEGATIVE = -1e30
LANES = 128
F32 = jnp.float32
BF16 = jnp.bfloat16
SCALE = (NOPE + ROPE) ** (-0.5)
LOG2E = math.log2(math.e)


NT = (((1,), (1,)), ((), ()))
TN = (((0,), (0,)), ((), ()))


def dot(a, b, dims=(((1,), (0,)), ((), ()))):
    return lax.dot_general(a, b, dims, preferred_element_type=F32)


def iota(shape, dim):
    return lax.broadcasted_iota(jnp.int32, shape, dim)


def one_hot(mask):
    return jnp.where(mask, 1.0, 0.0).astype(BF16)


def vmem(count):
    return [pl.BlockSpec(memory_space=pltpu.VMEM) for _ in range(count)]


def smem():
    return pl.BlockSpec(memory_space=pltpu.SMEM)


def call(body, name, out_shape, scratch, flops, args, scalars=0):
    return pl.pallas_call(
        body,
        out_shape=out_shape,
        in_specs=[smem()] * scalars + vmem(len(args) - scalars),
        out_specs=jax.tree.map(lambda _: pl.BlockSpec(memory_space=pltpu.VMEM), out_shape),
        scratch_shapes=scratch,
        cost_estimate=pl.CostEstimate(flops=int(flops), bytes_accessed=1 << 20, transcendentals=0),
        name=name,
    )(*args)


def struct(shape, dtype):
    return jax.ShapeDtypeStruct(shape, dtype)


def prep_body(q_up, kv_own, kv_other, rope_w, kv_down, wqp, wqs, wkt_own, wv_own, wkt_other, wv_other, wa):
    head = NOPE + ROPE
    half = ROPE // 2
    rows, cols = 4 * head, 4 * LANES
    r = iota((rows, cols), 0)
    lane = iota((rows, cols), 1)
    j = lane & (LANES - 1)
    base = (lane >> 7) * head + j
    straight = one_hot((r == base) & (j < head))
    turned = (j >= NOPE) & (j < head)
    low = j < NOPE + half
    other = base + jnp.where(low, half, -half)
    swapped = jnp.where(turned & (r == other), jnp.where(low, -1.0, 1.0), 0.0).astype(BF16)
    for g in range(q_up.shape[1] // rows):
        part = q_up[:, g * rows : (g + 1) * rows]
        wqp[:, g * cols : (g + 1) * cols] = dot(part, straight).astype(BF16)
        wqs[:, g * cols : (g + 1) * cols] = dot(part, swapped).astype(BF16)
    pair = 2 * (NOPE + VDIM)
    a = iota((LANES, pair), 0)
    b = iota((LANES, pair), 1)
    pick_k = one_hot(b == (a >> 6) * LANES + (a & (NOPE - 1)))
    a = iota((pair, LANES), 0)
    b = iota((pair, LANES), 1)
    pick_v = one_hot(a == (b >> 6) * LANES + NOPE + (b & (NOPE - 1)))
    for source, wkt, wv in ((kv_own, wkt_own, wv_own), (kv_other, wkt_other, wv_other)):
        for g in range(source.shape[1] // pair):
            part = source[:, g * pair : (g + 1) * pair]
            wkt[g * LANES : (g + 1) * LANES, :] = dot(pick_k, part, NT).astype(BF16)
            wv[:, g * LANES : (g + 1) * LANES] = dot(part, pick_v).astype(BF16)
    r = iota((ROPE, 2 * LANES), 0)
    lane = iota((ROPE, 2 * LANES), 1)
    j = (lane & (LANES - 1)) - NOPE
    inside = (j >= 0) & (j < ROPE)
    low = j < half
    first = lane < LANES
    want = jnp.where(first, j, j + jnp.where(low, half, -half))
    value = jnp.where(first, 1.0, jnp.where(low, -1.0, 1.0))
    pick_r = jnp.where(inside & (r == want), value, 0.0).astype(BF16)
    kv_rank = kv_down.shape[1]
    wa[:, :kv_rank] = kv_down[...]
    wa[:, kv_rank:] = dot(rope_w[...], pick_r).astype(BF16)


def spread(part, gain, fidx):
    wide = part[...].astype(F32)
    return wide, (wide * gain[fidx]).astype(BF16)


def feature(scal, index, feats):
    fidx = scal[8 + index]
    return fidx, pl.ds(pl.multiple_of(fidx * feats, LANES), feats)


def latent_body(columns, scal, *refs):
    parts = refs[: -8]
    gain, wa, kv_gain, cosf, sinf, chunk, factor_out, held = refs[-8:]
    rows, feats = parts[0].shape
    kv_rank = kv_gain.shape[1]
    half = rows // 2
    total = None
    squares = None
    for index, part in enumerate(parts):
        fidx, place = feature(scal, index, feats)
        wide, scaled = spread(part, gain, fidx)
        square = jnp.sum(wide * wide, axis=1, keepdims=True)
        product = dot(scaled, wa[place, :])
        total = product if total is None else total + product
        squares = square if squares is None else squares + square
    factor = lax.rsqrt(squares / (feats * len(parts)) + EPSILON)
    factor_out[...] = factor
    latent = total[:, :kv_rank] * factor
    mean = jnp.mean(latent * latent, axis=1, keepdims=True)
    held[...] = (latent * lax.rsqrt(mean + EPSILON) * kv_gain[...]).astype(BF16)
    core, x = scal[2], scal[1]
    chunk[:half, :] = held[pl.ds(pl.multiple_of(core * half, 16), half), :]
    straight = total[:, kv_rank : kv_rank + LANES] * factor
    swapped = total[:, kv_rank + LANES :] * factor
    turned = (straight * cosf[...] + swapped * sinf[...]).astype(BF16)
    keys = columns * half
    groups = (chunk.shape[0] - half) // ROPE
    width = groups * kv_rank
    token = iota((rows, width), 0) - core * half
    place = iota((rows, width), 1) - x * half
    pick = one_hot((token == place) & (place >= 0) & (place < half))
    moved = dot(turned, pick, TN).astype(BF16)
    for g in range(groups):
        chunk[half + g * ROPE : half + (g + 1) * ROPE, :] = moved[
            NOPE : NOPE + ROPE, g * kv_rank : (g + 1) * kv_rank
        ]


def query_body(scal, *refs):
    parts = refs[: -16]
    (gain, factor_ref, wq, q_gain, wqp, wqs, cosf, sinf, w_outer, w_inner, w_source,
     q_out, outer_out, driven_out, tail_out, scaled_all) = refs[-16:]
    rows, feats = parts[0].shape
    total = None
    for index, part in enumerate(parts):
        fidx, place = feature(scal, index, feats)
        _, scaled = spread(part, gain, fidx)
        scaled_all[:, place] = scaled
    scaled = scaled_all[...]
    factor = factor_ref[...]
    latent = dot(scaled, wq[...]) * factor
    mean = jnp.mean(latent * latent, axis=1, keepdims=True)
    normed = (latent * lax.rsqrt(mean + EPSILON) * q_gain[...]).astype(BF16)
    cosine, sine = cosf[...], sinf[...]
    straight = dot(normed, wqp[...])
    swapped = dot(normed, wqs[...])
    for h in range(q_out.shape[1] // LANES):
        span = slice(h * LANES, (h + 1) * LANES)
        q_out[:, span] = (straight[:, span] * cosine + swapped[:, span] * sine).astype(BF16)
    outer_out[...] = (dot(scaled, w_outer[...]) * factor).astype(BF16)
    inner = (dot(scaled, w_inner[...]) * factor).astype(BF16).astype(F32)
    source = (dot(scaled, w_source[...]) * factor).astype(BF16).astype(F32)
    driven = (inner * source).astype(BF16)
    driven_out[...] = driven
    tail_out[...] = driven[rows - tail_out.shape[0] :, :]


def conv_body(outer, driven, prior, taps, out, extended):
    rows = driven.shape[0]
    extended[:8, :] = prior[prior.shape[0] - 8 :, :].astype(F32)
    extended[8:, :] = driven[...].astype(F32)
    total = None
    for index in range(TAPS):
        start = 8 - (TAPS - 1) + index
        term = taps[index : index + 1, :].astype(F32) * extended[start : start + rows, :]
        total = term if total is None else total + term
    out[...] = (outer[...].astype(F32) * total).astype(BF16)


def unit_body(step, last, columns, scal, *refs):
    q_own, q_other = refs[:2]
    chunks = refs[2 : 2 + columns]
    rest = list(refs[2 + columns :])
    weights, rest = rest[:4], rest[4:]
    if step > 0:
        (acc_in, m_in, l_in), rest = rest[:3], rest[3:]
    if last:
        (out_own, lse_own, out_other), rest = rest[:3], rest[3:]
    else:
        (acc_out, m_out, l_out), rest = rest[:3], rest[3:]
    lat, keys_t, vals = rest[:3]
    if last:
        acc_out, m_out, l_out = rest[3:]
    rows = q_own.shape[0]
    half = rows // 2
    count = columns * half
    kv_rank = lat.shape[1]
    z, x, core = scal[0], scal[1], scal[2]
    local = q_own.shape[1] // LANES
    heads = 2 * local

    def work():
        rope = None
        for dx in range(columns):
            column = lax.rem(x + dx, columns)
            lat[pl.ds(pl.multiple_of(column * half, 16), half), :] = chunks[dx][:half, :]
            groups = (chunks[dx].shape[0] - half) // ROPE
            wide = [chunks[dx][half + g * ROPE : half + (g + 1) * ROPE, :] for g in range(groups)]
            wide = wide[0] if groups == 1 else jnp.concatenate(wide, axis=1)
            rope = wide if rope is None else rope + wide
        rope = rope[:, :count]
        block = lat[...]
        for side in range(2):
            made = dot(weights[2 * side][...], block, NT).astype(BF16)
            for h in range(local):
                keys_t[side * local + h, :NOPE, :] = made[h * NOPE : (h + 1) * NOPE, :]
                keys_t[side * local + h, NOPE : NOPE + ROPE, :] = rope
                keys_t[side * local + h, NOPE + ROPE :, :] = jnp.zeros(
                    (LANES - NOPE - ROPE, count), BF16
                )
            made = dot(block, weights[2 * side + 1][...]).astype(BF16)
            for p in range(local // 2):
                vals[side * (local // 2) + p, :, :LANES] = made[:, p * LANES : (p + 1) * LANES]
                vals[side * (local // 2) + p, :, LANES:] = jnp.ones((count, LANES), BF16)
        if step == 0:
            row = iota((rows, count), 0)
            key = iota((rows, count), 1)
            own = key - x * half
            allowed = (own < 0) | ((own < half) & (own + core * half <= row))
        lane = iota((rows, LANES), 1)
        low = lane < VDIM
        m_new_all = jnp.zeros((rows, LANES), F32)
        l_new_all = jnp.zeros((rows, LANES), F32)
        if step > 0:
            m_old_all = m_in[...]
            l_old_all = l_in[...]
        for p in range(heads // 2):
            side, inner = divmod(p, local // 2)
            q_ref = (q_own, q_other)[side]
            results, shrinks = [], []
            for e in range(2):
                h = 2 * p + e
                place = 2 * inner + e
                query = q_ref[:, place * LANES : (place + 1) * LANES]
                scores = dot(query, keys_t[h])
                if step == 0:
                    scores = jnp.where(allowed, scores, NEGATIVE)
                peak = jnp.max(scores, axis=1, keepdims=True)
                if step > 0:
                    before = m_old_all[:, h : h + 1]
                    peak = jnp.maximum(peak, before)
                    shrink = jnp.exp2((before - peak) * (SCALE * LOG2E))
                    shrinks.append(shrink)
                weight = jnp.exp2((scores - peak) * (SCALE * LOG2E)).astype(BF16)
                result = dot(weight, vals[p])
                sums = result[:, LANES:]
                if step > 0:
                    sums = sums + l_old_all * shrink
                m_new_all = jnp.where(lane == h, peak, m_new_all)
                l_new_all = jnp.where(lane == h, sums, l_new_all)
                results.append(result[:, :LANES])
            value = jnp.where(low, results[0], results[1])
            span = slice(p * LANES, (p + 1) * LANES)
            if step > 0:
                value = value + acc_in[:, span] * jnp.where(low, shrinks[0], shrinks[1])
            acc_out[:, span] = value
        m_out[...] = m_new_all
        l_out[...] = l_new_all

    if step == 0:
        work()
    else:
        pl.when(z >= step)(work)

        @pl.when(z < step)
        def _():
            acc_out[...] = acc_in[...]
            m_out[...] = m_in[...]
            l_out[...] = l_in[...]

    if last:
        lane = iota((rows, LANES), 1)
        low = lane < VDIM
        sums = jnp.where(lane < heads, l_out[...], 1.0)
        lse = m_out[...] * SCALE + jnp.log(sums)
        lse_own[...] = lse
        inverse = 1.0 / sums
        width = local * VDIM
        out_other[:, width:] = lse
        for p in range(heads // 2):
            ratio = jnp.where(low, inverse[:, 2 * p : 2 * p + 1], inverse[:, 2 * p + 1 : 2 * p + 2])
            value = acc_out[:, p * LANES : (p + 1) * LANES] * ratio
            side, inner = divmod(p, local // 2)
            target = (out_own, out_other)[side]
            target[:, inner * LANES : (inner + 1) * LANES] = value


def project_body(local, scal, own, lse_own, got, conv, w_attn, w_conv, keep, send, log_out, attended):
    rows = own.shape[0]
    width = local * VDIM
    groups, _, feats = keep.shape
    lane = iota((rows, LANES), 1)
    low = lane < VDIM
    mine = lse_own[...]
    theirs = pltpu.roll(got[:, width:], LANES - local, 1)
    peak = jnp.maximum(mine, theirs)
    a = jnp.exp(mine - peak)
    b = jnp.exp(theirs - peak)
    both = a + b
    log_total = peak + jnp.log(both)
    log_out[...] = jnp.transpose(log_total)[:local, :]
    a = a / both
    b = b / both
    for p in range(local // 2):
        span = slice(p * LANES, (p + 1) * LANES)
        first = jnp.where(low, a[:, 2 * p : 2 * p + 1], a[:, 2 * p + 1 : 2 * p + 2])
        second = jnp.where(low, b[:, 2 * p : 2 * p + 1], b[:, 2 * p + 1 : 2 * p + 2])
        attended[:, span] = (own[:, span] * first + got[:, span] * second).astype(BF16)
    heads = attended[...]
    channels = conv[...]
    for side, target in ((0, keep), (1, send)):
        for dy in range(groups):
            _, place = feature(scal, 2 * dy + side, feats)
            value = dot(heads, w_attn[:, place]) + dot(channels, w_conv[:, place])
            target[dy] = value.astype(BF16)


def body(columns, tokens, pre_gain, outer_gate_weight, inner_gate_weight, source_weight, conv_taps,
         q_down_weight, q_norm_gain, q_up_weight, kv_down_weight, rope_key_weight, kv_norm_gain,
         kv_up_weight, attn_out_weight, conv_out_weight, post_gain):
    n_sp, n_tp = lax.axis_size("sp"), lax.axis_size("tp")
    rows, feats = tokens.shape
    model = feats * n_tp
    half = rows // 2
    n_z, n_y = n_sp // columns, n_tp // 2
    local = q_up_weight.shape[1] // (NOPE + ROPE)
    kv_rank = kv_down_weight.shape[1]
    q_rank = q_down_weight.shape[1]
    channels = outer_gate_weight.shape[1]
    sp, tp = lax.axis_index("sp"), lax.axis_index("tp")
    z, x = sp // columns, sp % columns
    y, core = tp // 2, tp % 2

    def other_core(value):
        return lax.ppermute(value, "tp", [(i, i ^ 1) for i in range(n_tp)])

    def from_y(value, dy):
        pairs = [(i, (i // 2 - dy) % n_y * 2 + i % 2) for i in range(n_tp)]
        return lax.ppermute(value, "tp", pairs)

    def from_x(value, dx):
        pairs = [(s, s // columns * columns + (s % columns - dx) % columns) for s in range(n_sp)]
        return lax.ppermute(value, "sp", pairs)

    def from_z(value, dz):
        step = dz * columns
        return lax.ppermute(value, "sp", [(s, s + step) for s in range(n_sp - step)])

    order = [((y + dy) % n_y) * 2 + (core ^ dc) for dy in range(n_y) for dc in range(2)]
    scal = jnp.stack([z, x, core] + [jnp.int32(0)] * 5 + order).astype(jnp.int32)

    across = [from_y(tokens, dy) for dy in range(1, n_y)]
    parts = [tokens, other_core(tokens)]
    kv_up_other = other_core(kv_up_weight)
    for block in across:
        parts += [block, other_core(block)]

    positions = (sp * rows + jnp.arange(rows, dtype=jnp.int32)).astype(F32)
    freqs = THETA ** (-jnp.arange(0, ROPE, 2, dtype=F32) / ROPE)
    angles = positions[:, None] * freqs[None, :]
    cosine, sine = jnp.cos(angles), jnp.sin(angles)
    blank = jnp.zeros((rows, LANES - NOPE - ROPE), F32)
    cosf = jnp.concatenate([jnp.ones((rows, NOPE), F32), cosine, cosine, blank], axis=1)
    sinf = jnp.concatenate([jnp.zeros((rows, NOPE), F32), sine, sine, blank], axis=1)
    gain = pre_gain.reshape(n_tp, 1, feats)

    wide = local * LANES
    narrow = local * NOPE
    wqp, wqs, wkt_own, wv_own, wkt_other, wv_other, wa = call(
        prep_body,
        "prep",
        (
            struct((q_rank, wide), BF16),
            struct((q_rank, wide), BF16),
            struct((narrow, kv_rank), BF16),
            struct((kv_rank, narrow), BF16),
            struct((narrow, kv_rank), BF16),
            struct((kv_rank, narrow), BF16),
            struct((model, kv_rank + 2 * LANES), BF16),
        ),
        [],
        5e9,
        (q_up_weight, kv_up_weight, kv_up_other, rope_key_weight, kv_down_weight),
    )

    count = columns * half
    groups = -(-count // kv_rank)
    chunk, factor = call(
        functools.partial(latent_body, columns),
        "latent",
        (struct((half + ROPE * groups, kv_rank), BF16), struct((rows, 1), F32)),
        [pltpu.VMEM((rows, kv_rank), BF16)],
        2e9,
        (scal, *parts, gain, wa, kv_norm_gain.reshape(1, kv_rank), cosf, sinf),
        scalars=1,
    )
    own_column = [chunk] + [from_z(chunk, dz) for dz in range(1, n_z)]
    units = [[block] + [from_x(block, dx) for dx in range(1, columns)] for block in own_column]

    q_own, outer, driven, tail = call(
        query_body,
        "query",
        (
            struct((rows, wide), BF16),
            struct((rows, channels), BF16),
            struct((rows, channels), BF16),
            struct((16, channels), BF16),
        ),
        [pltpu.VMEM((rows, model), BF16)],
        4e9,
        (scal, *parts, gain, factor, q_down_weight, q_norm_gain.reshape(1, q_rank), wqp, wqs, cosf,
         sinf, outer_gate_weight, inner_gate_weight, source_weight),
        scalars=1,
    )
    q_other = other_core(q_own)
    prior = lax.ppermute(tail, "sp", [(s, s + 1) for s in range(n_sp - 1)])
    conv = call(
        conv_body,
        "conv",
        struct((rows, channels), BF16),
        [pltpu.VMEM((rows + 8, channels), F32)],
        1e8,
        (outer, driven, prior, conv_taps),
    )

    acc_shape = struct((rows, 2 * narrow), F32)
    stat_shape = struct((rows, LANES), F32)
    state = ()
    for step in range(n_z):
        last = step == n_z - 1
        carried = [acc_shape, stat_shape, stat_shape]
        scratch = [
            pltpu.VMEM((count, kv_rank), BF16),
            pltpu.VMEM((2 * local, LANES, count), BF16),
            pltpu.VMEM((local, count, 2 * LANES), BF16),
        ]
        if last:
            outs = (struct((rows, narrow), F32), stat_shape, struct((rows, narrow + LANES), F32))
            scratch += [pltpu.VMEM(s.shape, s.dtype) for s in carried]
        else:
            outs = tuple(carried)
        state = call(
            functools.partial(unit_body, step, last, columns),
            "unit",
            outs,
            scratch,
            4e9,
            (scal, q_own, q_other, *units[step], wkt_own, wv_own, wkt_other, wv_other, *state),
            scalars=1,
        )
    out_own, lse_own, out_other = state
    got = other_core(out_other)

    keep, send, log_total = call(
        functools.partial(project_body, local),
        "project",
        (
            struct((n_y, rows, feats), BF16),
            struct((n_y, rows, feats), BF16),
            struct((local, rows), F32),
        ),
        [pltpu.VMEM((rows, narrow), BF16)],
        2e9,
        (scal, out_own, lse_own, got, conv, attn_out_weight, conv_out_weight),
        scalars=1,
    )
    received = other_core(send)
    both = keep.astype(F32) + received.astype(F32)
    total = both[0]
    crossing = both.astype(BF16)
    for dy in range(1, n_y):
        total = total + from_y(crossing[n_y - dy], dy).astype(F32)
    squares = jnp.sum(total * total, axis=1)
    row_squares = squares
    for shift in range(1, n_tp):
        row_squares = row_squares + lax.ppermute(
            squares, "tp", [(i, (i + shift) % n_tp) for i in range(n_tp)]
        )
    mixed = total * lax.rsqrt(row_squares / model + EPSILON)[:, None] * post_gain
    return (mixed.astype(BF16), log_total)


def columns_of(mesh):
    devices = mesh.devices
    first = devices.reshape(-1)[0]
    if not hasattr(first, "coords"):
        return 2
    axis = list(mesh.axis_names).index("sp")
    line = devices.swapaxes(0, axis)
    line = line.reshape(line.shape[0], -1)[:, 0]
    return len({device.coords[0] for device in line})


def solution(mesh):
    placed = (
        P("sp", "tp"),
        P(),
        P(None, "tp"),
        P(None, "tp"),
        P(None, "tp"),
        P(None, "tp"),
        P(),
        P(),
        P(None, "tp"),
        P(),
        P(),
        P(),
        P(None, "tp"),
        P("tp", None),
        P("tp", None),
        P("tp"),
    )
    return jax.shard_map(
        functools.partial(body, columns_of(mesh)),
        mesh=mesh,
        in_specs=placed,
        out_specs=(P("sp", "tp"), P("tp", "sp")),
        check_vma=False,
    )
```
